256 devices in a mesh: kv: 16 (over y, x), tp: 16 (over z, core).
Axes of the slice: x: 4, y: 4, z: 8, core: 2. Of those that a mesh axis runs over, the one named last changes fastest.
Arguments:
- tokens: bfloat16 [256, 4096], P('kv', 'tp'), may hold values from -6 to 6
- attn_gain: float32 [4096], replicated, may hold values from 0.1 to 1.9
- w_query: bfloat16 [4096, 2048], P(None, 'tp'), may hold values from -0.09375 to 0.09375
- w_key: bfloat16 [4096, 2048], P(None, 'tp'), may hold values from -0.09375 to 0.09375
- w_value: bfloat16 [4096, 2048], P(None, 'tp'), may hold values from -0.09375 to 0.09375
- w_outgate: bfloat16 [4096, 2048], P(None, 'tp'), may hold values from -0.09375 to 0.09375
- w_rates: bfloat16 [2, 4096, 16], P(None, None, 'tp'), may hold values from -0.09375 to 0.09375
- head_rate: float32 [16], P('tp'), may hold values from 0.02 to 2
- head_gain: float32 [2048], P('tp'), may hold values from 0.1 to 1.9
- w_out: bfloat16 [2048, 4096], P('tp'), may hold values from -0.125 to 0.125
- state: float32 [256, 16, 128, 128], P('kv', 'tp'), may hold values from -2.4 to 2.4
- mlp_gain: float32 [4096], replicated, may hold values from 0.1 to 1.9
- w_gate: bfloat16 [4096, 11264], P(None, ('kv', 'tp')), may hold values from -0.09375 to 0.09375
- w_up: bfloat16 [4096, 11264], P(None, ('kv', 'tp')), may hold values from -0.09375 to 0.09375
- w_down: bfloat16 [4096, 11264], P(None, ('kv', 'tp')), may hold values from -0.25 to 0.25
Outputs:
- result: bfloat16 [256, 4096], P('kv', 'tp')
- new_state: float32 [256, 16, 128, 128], P('kv', 'tp')
The draws below stay inside these ranges and needn't reach their ends.
All inputs are finite; a program needn't handle non-finite values.
Results may differ from the reference program's by a relative error of at most 0.014.
Values may be sent and summed in bfloat16 or wider, within the bound.
A program may use at most 64 MiB of HBM per device.

```python
import math
import jax
import jax.numpy as jnp
from jax import lax

D = 4096
H = 16
HEAD = 128
FF = 11264
BATCH = 256


def with_spikes(entries, key, source, target, shards_of, factor):
    owner, partner = [(jnp.arange(entries.shape[axis_at]) // (entries.shape[axis_at] // shards_of)).reshape([-1 if axis == axis_at else 1 for axis in range(entries.ndim)]) for axis_at in (source, target)]
    chosen = jax.random.permutation(key, shards_of)[partner]
    strong = (owner == chosen) | (owner == (partner + shards_of // 2) % shards_of)
    return jnp.where(strong, factor * entries, entries)


def shard_levels(key, shape, cuts, least, top_value):
    level = 1.0
    for axis_at, parts in cuts:
        steps = jax.random.uniform(jax.random.fold_in(jax.random.fold_in(key, 6), axis_at), (parts,), jnp.float32, least / len(cuts), top_value / len(cuts))
        level = level * jnp.repeat(jnp.exp(steps), shape[axis_at] // parts).reshape((-1,) + (1,) * (len(shape) - 1 - axis_at))
    return level


def scatter_about(key, dims, width, reach, shards=(), kind=jnp.bfloat16):
    array = jax.random.normal(key, dims, jnp.float32) * width
    if len(shards) > 0:
        array = shard_levels(key, dims, shards, -0.22, 0.18) * array
    return jnp.clip(array, min=-reach, max=reach).astype(kind)


def heavy_noise(key, dims, width, most, split, heavy, dtype=jnp.bfloat16):
    array = width * jax.random.normal(key, dims, jnp.float32)
    if split:
        array = array * shard_levels(key, dims, split, -0.22, 0.18)
    return jnp.clip(with_spikes(array, jax.random.fold_in(key, 3), *heavy), -most, most).astype(dtype)


def setup_inputs(seed: int = 0) -> dict:
    splits = jax.random.split(jax.random.key(seed), 16)
    return {
        "tokens": scatter_about(splits[0], (BATCH, D), 1.0, 6.0, ((0, 16), (1, 16))),
        "attn_gain": jnp.clip(1.0 + 0.18 * jax.random.normal(splits[1], (D,), jnp.float32), 0.1, 1.9),
        "w_query": scatter_about(splits[2], (D, H * HEAD), D ** -0.5, 0.09375, ((1, 16),)),
        "w_key": scatter_about(splits[3], (D, H * HEAD), D ** -0.5, 0.09375, ((1, 16),)),
        "w_value": scatter_about(splits[4], (D, H * HEAD), D ** -0.5, 0.09375, ((1, 16),)),
        "w_outgate": scatter_about(splits[5], (D, H * HEAD), D ** -0.5, 0.09375, ((1, 16),)),
        "w_rates": scatter_about(splits[6], (2, D, H), D ** -0.5, 0.09375, ((2, 16),)),
        "head_rate": jnp.clip(jnp.exp(math.log(2.0) - 4.6051702 * jax.random.uniform(splits[7], (H,), jnp.float32) ** shard_levels(splits[7], (H,), ((0, 16),), -0.2, 0.2)), 0.02, 2.0),
        "head_gain": jnp.clip(1.0 + 0.18 * jax.random.normal(splits[8], (H * HEAD,), jnp.float32), 0.1, 1.9),
        "w_out": scatter_about(splits[9], (H * HEAD, D), (H * HEAD) ** -0.5, 0.125, ((0, 16),)),
        "state": scatter_about(splits[10], (BATCH, H, HEAD, HEAD), 0.3, 2.4, ((0, 16), (1, 16)), jnp.float32),
        "mlp_gain": jnp.clip(1.0 + 0.18 * jax.random.normal(splits[11], (D,), jnp.float32), 0.1, 1.9),
        "w_gate": scatter_about(splits[12], (D, FF), D ** -0.5, 0.09375, ((1, 256),)),
        "w_up": scatter_about(splits[13], (D, FF), D ** -0.5, 0.09375, ((1, 256),)),
        "w_down": heavy_noise(splits[14], (D, FF), FF ** -0.5, 0.25, ((1, 256),), (1, 0, 256, 6.0)),
    }


EPS = 1e-06

def row_norm(values, gain):
    floats = values.astype(jnp.float32)
    scaled = floats * lax.rsqrt(lax.optimization_barrier(jnp.mean(floats * floats, axis=-1, keepdims=True)) + EPS)
    return (scaled * gain.astype(jnp.float32)).astype(jnp.bfloat16)

def reference(tokens, attn_gain, w_query, w_key, w_value, w_outgate, w_rates, head_rate, head_gain, w_out, state, mlp_gain, w_gate, w_up, w_down):
    count = tokens.shape[0]
    normed = row_norm(tokens, attn_gain)
    query = jnp.dot(normed, w_query, preferred_element_type=jnp.float32).reshape(count, H, HEAD)
    key = jnp.dot(normed, w_key, preferred_element_type=jnp.float32).reshape(count, H, HEAD)
    value = jnp.dot(normed, w_value, preferred_element_type=jnp.float32).reshape(count, H, HEAD)
    gate_in = jnp.dot(normed, w_outgate, preferred_element_type=jnp.float32).reshape(count, H, HEAD)
    write_raw = jnp.dot(normed, w_rates[0], preferred_element_type=jnp.float32)
    decay_raw = jnp.dot(normed, w_rates[1], preferred_element_type=jnp.float32)
    unit_query = query * lax.rsqrt(lax.optimization_barrier(jnp.sum(query * query, axis=-1, keepdims=True)) + EPS) * HEAD ** (-0.5)
    unit_key = key * lax.rsqrt(lax.optimization_barrier(jnp.sum(key * key, axis=-1, keepdims=True)) + EPS)
    strength = jax.nn.sigmoid(write_raw)
    fade = jnp.exp(-head_rate * jax.nn.softplus(decay_raw))
    carried = state * fade[:, :, None, None]
    fresh = strength[:, :, None] * (value - jnp.einsum('bhi,bhiv->bhv', unit_key, carried))
    new_state = carried + unit_key[:, :, :, None] * fresh[:, :, None, :]
    readout = jnp.einsum('bhi,bhiv->bhv', unit_query, new_state)
    normed_out = readout * lax.rsqrt(lax.optimization_barrier(jnp.mean(readout * readout, axis=-1, keepdims=True)) + EPS)
    mixed = (normed_out * head_gain.reshape(H, HEAD) * jax.nn.silu(gate_in)).astype(jnp.bfloat16).reshape(count, H * HEAD)
    projected = jnp.dot(mixed, w_out, preferred_element_type=jnp.float32)
    residual = (tokens.astype(jnp.float32) + projected).astype(jnp.bfloat16)
    normed_mlp = row_norm(residual, mlp_gain)
    gate_pre = jnp.dot(normed_mlp, w_gate, preferred_element_type=jnp.float32)
    up_pre = jnp.dot(normed_mlp, w_up, preferred_element_type=jnp.float32)
    hidden = (jax.nn.silu(gate_pre) * up_pre).astype(jnp.bfloat16)
    down = lax.dot_general(hidden, w_down, (((1,), (1,)), ((), ())), preferred_element_type=jnp.float32)
    result = (residual.astype(jnp.float32) + down).astype(jnp.bfloat16)
    return (result, new_state)
```

```python
import math

import jax
import jax.numpy as jnp
from jax import lax
from jax.experimental import pallas as pl
from jax.experimental.pallas import tpu as pltpu
from jax.sharding import PartitionSpec as P

EPS = 1e-06
MESH = pl.DeviceIdType.MESH
F32 = jnp.float32
BF16 = jnp.bfloat16


def layer_kernel(
    n_side,
    n_z,
    tok_hbm,
    again_ref,
    wq_hbm,
    wk_hbm,
    wv_hbm,
    wo_hbm,
    wrates_ref,
    hrate_ref,
    hgain_ref,
    wout_hbm,
    state_hbm,
    mgain_ref,
    wgate_hbm,
    wup_hbm,
    wdown_hbm,
    result_ref,
    ns_hbm,
    tok_own,
    tok_all,
    wqkvg,
    wout,
    state,
    ns,
    pred,
    own_w,
    far_w,
    gu,
    wd,
    part1,
    recv1,
    ag,
    ex_out,
    ex_in,
    pb,
    ra1,
    ra2,
    rb1,
    rb2,
    mid_a,
    mid_b,
    zout,
    zin,
    local_sem,
    loc_w_sem,
    far_send_sem,
    far_recv_sem,
    tok_send_sem,
    tok_recv_sem,
    p1_send_sem,
    p1_recv_sem,
    agz_send_sem,
    agz_recv_sem,
    ag_send_sem,
    ag_recv_sem,
    ex_send_sem,
    ex_recv_sem,
    r1_send_sem,
    r1_recv_sem,
    r2_send_sem,
    r2_recv_sem,
    rz_send_sem,
    rz_recv_sem,
):
    n_tp = 2 * n_z
    half = n_z // 2
    rows, fpd = tok_own.shape
    head = hgain_ref.shape[1]
    units = wgate_hbm.shape[0]
    upad = gu.shape[0] // 4
    me_k = lax.axis_index("kv")
    me_t = lax.axis_index("tp")
    my_y, my_x = me_k // n_side, lax.rem(me_k, n_side)
    my_z, my_c = me_t // 2, lax.rem(me_t, 2)
    partner = me_t + 1 - 2 * my_c

    def z_at(d):
        return lax.rem(my_z + d, n_z)

    def y_at(d):
        return lax.rem(my_y + d, n_side)

    def x_at(d):
        return lax.rem(my_x + d, n_side)

    def tp_id(t):
        return {"tp": t}

    def kv_id(y, x):
        return {"kv": y * n_side + x}

    def remote(src, dst, send, recv, device):
        return pltpu.make_async_remote_copy(
            src_ref=src,
            dst_ref=dst,
            send_sem=send,
            recv_sem=recv,
            device_id=device,
            device_id_type=MESH,
        )

    near = [0]
    for d in range(1, n_z // 2):
        near += [d, n_z - d]
    near += [n_z // 2]
    others = [(d, c) for d in near for c in (0, 1)][1:]

    def tp_at(d, flip):
        c = (1 - my_c) if flip else my_c
        return z_at(d) * 2 + c

    tok_copy = pltpu.make_async_copy(tok_hbm, tok_own, local_sem.at[0])
    tok_copy.start()
    w_copies = []
    for j, src in enumerate((wq_hbm, wk_hbm, wv_hbm, wo_hbm)):
        cp = pltpu.make_async_copy(
            src, wqkvg.at[:, pl.ds(j * head, head)], local_sem.at[1 + j]
        )
        cp.start()
        w_copies.append(cp)
    state_copy = pltpu.make_async_copy(state_hbm, state, local_sem.at[5])
    state_copy.start()
    wout_copy = pltpu.make_async_copy(wout_hbm, wout, local_sem.at[6])
    wout_copy.start()
    own_copies = []
    mats = (wgate_hbm, wup_hbm, wdown_hbm)
    for j, src in enumerate(mats):
        for zz in range(n_z):
            cols = pl.ds(pl.multiple_of((2 * zz + my_c) * fpd, fpd), fpd)
            cp = pltpu.make_async_copy(src.at[:, cols], own_w.at[j, zz], loc_w_sem.at[j, zz])
            cp.start()
            own_copies.append(cp)

    barrier = pltpu.get_barrier_semaphore()
    for d, flip in others:
        pl.semaphore_signal(
            barrier, inc=1, device_id=tp_id(tp_at(d, flip)), device_id_type=MESH
        )
    for d in range(1, n_side):
        pl.semaphore_signal(
            barrier, inc=1, device_id=kv_id(y_at(d), my_x), device_id_type=MESH
        )
        pl.semaphore_signal(
            barrier, inc=1, device_id=kv_id(my_y, x_at(d)), device_id_type=MESH
        )
    pl.semaphore_wait(barrier, len(others) + 2 * (n_side - 1))

    tok_copy.wait()
    tok_sends = []
    for d, flip in reversed(others):
        to = tp_at(d, flip)
        cp = remote(
            tok_own, tok_all.at[me_t], tok_send_sem.at[to], tok_recv_sem.at[me_t], tp_id(to)
        )
        cp.start()
        tok_sends.append(cp)

    far_sends = []
    for j, src in enumerate(mats):
        for zz in range(n_z):
            cols = pl.ds(pl.multiple_of((2 * zz + 1 - my_c) * fpd, fpd), fpd)
            cp = remote(
                src.at[:, cols],
                far_w.at[j, zz],
                far_send_sem.at[j, zz],
                far_recv_sem.at[j, zz],
                tp_id(partner),
            )
            cp.start()
            far_sends.append(cp)

    zero_rows = jnp.zeros((upad - units, fpd), BF16)
    for cp in own_copies:
        cp.wait()
    for cp in far_sends:
        cp.wait_recv()
    for zz in range(n_z):
        cols = pl.ds(pl.multiple_of((2 * zz + my_c) * fpd, fpd), fpd)
        gain = mgain_ref[:, cols]
        here = slice(zz * fpd, (zz + 1) * fpd)
        for j in range(2):
            for s, src in enumerate((own_w, far_w)):
                row = (2 * j + s) * upad
                scaled = (src[j, zz].astype(F32) * gain).astype(BF16)
                gu[row : row + units, here] = scaled
                gu[row + units : row + upad, here] = zero_rows
        for s, src in enumerate((own_w, far_w)):
            wd[s * upad : s * upad + units, here] = src[2, zz]
            wd[s * upad + units : (s + 1) * upad, here] = zero_rows

    for cp in w_copies:
        cp.wait()
    acc = jnp.zeros((rows, 4 * head), F32)
    square = jnp.zeros((rows, fpd), F32)
    write_sum = jnp.zeros((rows, fpd), F32)
    decay_sum = jnp.zeros((rows, fpd), F32)
    for i, (d, flip) in enumerate([(0, 0)] + others):
        t = tp_at(d, flip)
        if i == 0:
            piece = tok_own[...].astype(F32)
        else:
            remote(
                tok_own, tok_all.at[t], tok_send_sem.at[t], tok_recv_sem.at[t], tp_id(t)
            ).wait_recv()
            piece = tok_all[t].astype(F32)
        cols = pl.ds(pl.multiple_of(t * fpd, fpd), fpd)
        square += piece * piece
        lhs = (piece * again_ref[:, cols]).astype(BF16)
        lhs32 = lhs.astype(F32)
        write_sum += lhs32 * wrates_ref[0:1, cols].astype(F32)
        decay_sum += lhs32 * wrates_ref[1:2, cols].astype(F32)
        acc += jnp.dot(lhs, wqkvg[cols, :], preferred_element_type=F32)
    count = fpd * n_tp
    scale = lax.rsqrt(jnp.sum(square, axis=1, keepdims=True) / count + EPS)
    acc = acc * scale
    query = acc[:, 0:head]
    key = acc[:, head : 2 * head]
    value = acc[:, 2 * head : 3 * head]
    gate_in = acc[:, 3 * head : 4 * head]
    write_raw = jnp.sum(write_sum, axis=1, keepdims=True) * scale
    decay_raw = jnp.sum(decay_sum, axis=1, keepdims=True) * scale
    unit_query = query * (
        lax.rsqrt(jnp.sum(query * query, axis=1, keepdims=True) + EPS) * head ** (-0.5)
    )
    unit_key = key * lax.rsqrt(jnp.sum(key * key, axis=1, keepdims=True) + EPS)
    strength = 1.0 / (1.0 + jnp.exp(-write_raw))
    softplus = jnp.maximum(decay_raw, 0.0) + jnp.log(1.0 + jnp.exp(-jnp.abs(decay_raw)))
    fade = jnp.exp(-hrate_ref[0] * softplus)

    state_copy.wait()
    stacked = jnp.concatenate(
        [unit_key, unit_query, jnp.zeros((head - 2 * rows, head), F32)], axis=0
    )
    turned = stacked.T
    for b in range(rows):
        block = state[b]
        pred[0, b : b + 1, :] = jnp.sum(turned[:, b : b + 1] * block, axis=0, keepdims=True)
        pred[1, b : b + 1, :] = jnp.sum(
            turned[:, rows + b : rows + b + 1] * block, axis=0, keepdims=True
        )
    fresh = strength * (value - fade * pred[0])
    overlap = jnp.sum(unit_query * unit_key, axis=1, keepdims=True)
    readout = fade * pred[1] + overlap * fresh
    normed_out = readout * lax.rsqrt(
        jnp.sum(readout * readout, axis=1, keepdims=True) / head + EPS
    )
    mixed = (
        normed_out * hgain_ref[...] * (gate_in / (1.0 + jnp.exp(-gate_in)))
    ).astype(BF16)

    wout_copy.wait()
    for t in range(n_tp):
        part1[t] = jnp.dot(
            mixed, wout[:, t * fpd : (t + 1) * fpd], preferred_element_type=F32
        ).astype(BF16)
    p1_sends = []
    for d, flip in reversed(others):
        to = tp_at(d, flip)
        cp = remote(
            part1.at[to], recv1.at[me_t], p1_send_sem.at[to], p1_recv_sem.at[me_t], tp_id(to)
        )
        cp.start()
        p1_sends.append(cp)

    for b in range(rows):
        ns[b] = fade[b : b + 1, :] * state[b] + turned[:, b : b + 1] * fresh[b : b + 1, :]
    ns_copy = pltpu.make_async_copy(ns, ns_hbm, local_sem.at[7])
    ns_copy.start()

    total = tok_own[...].astype(F32) + part1[me_t].astype(F32)
    for d, flip in others:
        t = tp_at(d, flip)
        remote(
            part1.at[t], recv1.at[t], p1_send_sem.at[t], p1_recv_sem.at[t], tp_id(t)
        ).wait_recv()
        total += recv1[t].astype(F32)
    residual = total.astype(BF16)
    ag[my_y, my_x, my_z] = residual

    agz_sends = []
    mine = ag.at[my_y, my_x, my_z]
    for d in reversed(near[1:]):
        zz = z_at(d)
        cp = remote(
            mine, mine, agz_send_sem.at[zz], agz_recv_sem.at[my_z], tp_id(zz * 2 + my_c)
        )
        cp.start()
        agz_sends.append(cp)
    for d in near[1:]:
        zz = z_at(d)
        slot = ag.at[my_y, my_x, zz]
        remote(
            slot, slot, agz_send_sem.at[zz], agz_recv_sem.at[zz], tp_id(zz * 2 + my_c)
        ).wait_recv()

    low, high = pl.ds(0, half), pl.ds(half, half)

    def spread(h, y, x, along_x, d, first=False):
        block = ag.at[y, x, (low, high)[h]]
        to = kv_id(my_y, x_at(d)) if along_x else kv_id(y_at(d), my_x)
        sent = ag_send_sem.at[2, h, 0, d] if first else ag_send_sem.at[h, y, x, d]
        return remote(block, block, sent, ag_recv_sem.at[h, y, x], to)

    def arrive(h, y, x):
        block = ag.at[y, x, (low, high)[h]]
        remote(
            block, block, ag_send_sem.at[h, y, x, 0], ag_recv_sem.at[h, y, x], kv_id(y, x)
        ).wait_recv()

    spread_order = [2, 1, 3] if n_side == 4 else list(range(1, n_side))
    arrive_order = [1, 3, 2] if n_side == 4 else list(range(1, n_side))
    ag_sends = []
    for d in spread_order:
        for h, along_x in ((0, True), (1, False)):
            cp = spread(h, my_y, my_x, along_x, d, first=True)
            cp.start()
            ag_sends.append(cp)
    for d in spread_order:
        for h, along_x in ((0, False), (1, True)):
            cp = spread(h, my_y, my_x, along_x, d)
            cp.start()
            ag_sends.append(cp)
    for d in arrive_order:
        arrive(0, my_y, x_at(d))
        for e in spread_order:
            cp = spread(0, my_y, x_at(d), False, e)
            cp.start()
            ag_sends.append(cp)
        arrive(1, y_at(d), my_x)
        for e in spread_order:
            cp = spread(1, y_at(d), my_x, True, e)
            cp.start()
            ag_sends.append(cp)
    for d in arrive_order:
        arrive(0, y_at(d), my_x)
        arrive(1, my_y, x_at(d))
    for d in arrive_order:
        for e in arrive_order:
            arrive(0, y_at(d), x_at(e))
            arrive(1, y_at(d), x_at(e))

    batch = rows * n_side * n_side
    acc2 = jnp.zeros((batch, 4 * upad), F32)
    sq2 = jnp.zeros((batch, 128), F32)
    for zz in range(n_z):
        lhs = ag[:, :, zz].reshape(batch, fpd)
        wide = lhs.astype(F32)
        wide = wide * wide
        for q in range(fpd // 128):
            sq2 += wide[:, q * 128 : (q + 1) * 128]
        acc2 += lax.dot_general(
            lhs,
            gu[:, zz * fpd : (zz + 1) * fpd],
            (((1,), (1,)), ((), ())),
            preferred_element_type=F32,
        )
    ex_out[0] = acc2[:, : 2 * upad]
    ex_out[1] = acc2[:, 2 * upad :]
    ex_out[2] = sq2
    ex_copy = remote(ex_out, ex_in, ex_send_sem, ex_recv_sem, tp_id(partner))
    ex_copy.start()
    ex_copy.wait_recv()
    row_scale = lax.rsqrt(
        jnp.sum(ex_out[2] + ex_in[2], axis=1, keepdims=True) / count + EPS
    )
    gate_far = pltpu.roll(ex_in[0], upad, 1)
    up_far = pltpu.roll(ex_in[1], upad, 1)
    gate_pre = (ex_out[0] + gate_far) * row_scale
    up_pre = (ex_out[1] + up_far) * row_scale
    hidden = (gate_pre / (1.0 + jnp.exp(-gate_pre)) * up_pre).astype(BF16)

    for zz in range(n_z):
        down = jnp.dot(hidden, wd[:, zz * fpd : (zz + 1) * fpd], preferred_element_type=F32)
        pb[:, :, zz] = down.astype(BF16).reshape(n_side, n_side, rows, fpd)
    r1_sends = []
    for d in spread_order:
        yy, xx = y_at(d), x_at(d)
        cp = remote(
            pb.at[yy, :, low], ra1.at[my_y], r1_send_sem.at[0, yy], r1_recv_sem.at[0, my_y],
            kv_id(yy, my_x),
        )
        cp.start()
        r1_sends.append(cp)
        cp = remote(
            pb.at[:, xx, high], rb1.at[my_x], r1_send_sem.at[1, xx], r1_recv_sem.at[1, my_x],
            kv_id(my_y, xx),
        )
        cp.start()
        r1_sends.append(cp)
    for d in arrive_order:
        yy, xx = y_at(d), x_at(d)
        remote(
            pb.at[yy, :, low], ra1.at[yy], r1_send_sem.at[0, yy], r1_recv_sem.at[0, yy],
            kv_id(yy, my_x),
        ).wait_recv()
        remote(
            pb.at[:, xx, high], rb1.at[xx], r1_send_sem.at[1, xx], r1_recv_sem.at[1, xx],
            kv_id(my_y, xx),
        ).wait_recv()
    r2_sends = []
    for e in spread_order + [0]:
        yy, xx = y_at(e), x_at(e)
        sum_a = pb[my_y, xx, 0:half].astype(F32)
        sum_b = pb[yy, my_x, half:n_z].astype(F32)
        for d in range(1, n_side):
            sum_a += ra1[y_at(d), xx].astype(F32)
            sum_b += rb1[x_at(d), yy].astype(F32)
        mid_a[xx] = sum_a.astype(BF16)
        mid_b[yy] = sum_b.astype(BF16)
        if e:
            cp = remote(
                mid_a.at[xx], ra2.at[my_x], r2_send_sem.at[0, xx], r2_recv_sem.at[0, my_x],
                kv_id(my_y, xx),
            )
            cp.start()
            r2_sends.append(cp)
            cp = remote(
                mid_b.at[yy], rb2.at[my_y], r2_send_sem.at[1, yy], r2_recv_sem.at[1, my_y],
                kv_id(yy, my_x),
            )
            cp.start()
            r2_sends.append(cp)
    sum_a = mid_a[my_x].astype(F32)
    sum_b = mid_b[my_y].astype(F32)
    for d in arrive_order:
        yy, xx = y_at(d), x_at(d)
        remote(
            mid_a.at[xx], ra2.at[xx], r2_send_sem.at[0, xx], r2_recv_sem.at[0, xx],
            kv_id(my_y, xx),
        ).wait_recv()
        sum_a += ra2[xx].astype(F32)
        remote(
            mid_b.at[yy], rb2.at[yy], r2_send_sem.at[1, yy], r2_recv_sem.at[1, yy],
            kv_id(yy, my_x),
        ).wait_recv()
        sum_b += rb2[yy].astype(F32)
    zout[0:half] = sum_a.astype(BF16)
    zout[half:n_z] = sum_b.astype(BF16)
    rz_sends = []
    for d in reversed(near[1:]):
        zz = z_at(d)
        cp = remote(
            zout.at[zz], zin.at[my_z], rz_send_sem.at[zz], rz_recv_sem.at[my_z],
            tp_id(zz * 2 + my_c),
        )
        cp.start()
        rz_sends.append(cp)
    out = residual.astype(F32) + zout[my_z].astype(F32)
    for d in near[1:]:
        zz = z_at(d)
        remote(
            zout.at[zz], zin.at[zz], rz_send_sem.at[zz], rz_recv_sem.at[zz],
            tp_id(zz * 2 + my_c),
        ).wait_recv()
        out += zin[zz].astype(F32)
    result_ref[...] = out.astype(BF16)

    ns_copy.wait()
    for cp in (
        tok_sends + far_sends + p1_sends + agz_sends + ag_sends + r1_sends + r2_sends + rz_sends
    ):
        cp.wait_send()
    ex_copy.wait_send()


def solution(mesh):
    n_kv, n_tp = mesh.shape["kv"], mesh.shape["tp"]
    n_side = math.isqrt(n_kv)
    n_z = n_tp // 2
    half = n_z // 2

    def body(
        tokens,
        attn_gain,
        w_query,
        w_key,
        w_value,
        w_outgate,
        w_rates,
        head_rate,
        head_gain,
        w_out,
        state,
        mlp_gain,
        w_gate,
        w_up,
        w_down,
    ):
        rows, fpd = tokens.shape
        feats = fpd * n_tp
        head = w_query.shape[1]
        units = w_gate.shape[1]
        upad = 64
        batch = rows * n_kv
        plane = fpd * n_z
        any_spec = pl.BlockSpec(memory_space=pl.ANY)
        vmem = pl.BlockSpec(memory_space=pltpu.VMEM)
        smem = pl.BlockSpec(memory_space=pltpu.SMEM)
        dma = pltpu.SemaphoreType.DMA

        def kernel(*refs):
            layer_kernel(n_side, n_z, *refs)

        result, new_state = pl.pallas_call(
            kernel,
            name="layer",
            out_shape=(
                jax.ShapeDtypeStruct((rows, fpd), BF16),
                jax.ShapeDtypeStruct((rows, head, head), F32),
            ),
            in_specs=[
                any_spec,
                vmem,
                any_spec,
                any_spec,
                any_spec,
                any_spec,
                vmem,
                smem,
                vmem,
                any_spec,
                any_spec,
                vmem,
                any_spec,
                any_spec,
                any_spec,
            ],
            out_specs=(vmem, any_spec),
            scratch_shapes=[
                pltpu.VMEM((rows, fpd), BF16),
                pltpu.VMEM((n_tp, rows, fpd), BF16),
                pltpu.VMEM((feats, 4 * head), BF16),
                pltpu.VMEM((head, feats), BF16),
                pltpu.VMEM((rows, head, head), F32),
                pltpu.VMEM((rows, head, head), F32),
                pltpu.VMEM((2, rows, head), F32),
                pltpu.VMEM((3, n_z, units, fpd), BF16),
                pltpu.VMEM((3, n_z, units, fpd), BF16),
                pltpu.VMEM((4 * upad, plane), BF16),
                pltpu.VMEM((2 * upad, plane), BF16),
                pltpu.VMEM((n_tp, rows, fpd), BF16),
                pltpu.VMEM((n_tp, rows, fpd), BF16),
                pltpu.VMEM((n_side, n_side, n_z, rows, fpd), BF16),
                pltpu.VMEM((3, batch, 128), F32),
                pltpu.VMEM((3, batch, 128), F32),
                pltpu.VMEM((n_side, n_side, n_z, rows, fpd), BF16),
                pltpu.VMEM((n_side, n_side, half, rows, fpd), BF16),
                pltpu.VMEM((n_side, half, rows, fpd), BF16),
                pltpu.VMEM((n_side, n_side, half, rows, fpd), BF16),
                pltpu.VMEM((n_side, half, rows, fpd), BF16),
                pltpu.VMEM((n_side, half, rows, fpd), BF16),
                pltpu.VMEM((n_side, half, rows, fpd), BF16),
                pltpu.VMEM((n_z, rows, fpd), BF16),
                pltpu.VMEM((n_z, rows, fpd), BF16),
                dma((8,)),
                dma((3, n_z)),
                dma((3, n_z)),
                dma((3, n_z)),
                dma((n_tp,)),
                dma((n_tp,)),
                dma((n_tp,)),
                dma((n_tp,)),
                dma((n_z,)),
                dma((n_z,)),
                dma((3, n_side, n_side, n_side)),
                dma((2, n_side, n_side)),
                dma,
                dma,
                dma((2, n_side)),
                dma((2, n_side)),
                dma((2, n_side)),
                dma((2, n_side)),
                dma((n_z,)),
                dma((n_z,)),
            ],
            compiler_params=pltpu.CompilerParams(
                collective_id=0,
                has_side_effects=True,
                vmem_limit_bytes=60 * 1024 * 1024,
            ),
        )(
            tokens,
            attn_gain.reshape(1, feats),
            w_query,
            w_key,
            w_value,
            w_outgate,
            w_rates.reshape(2, feats),
            head_rate,
            head_gain.reshape(1, head),
            w_out,
            state.reshape(rows, head, head),
            mlp_gain.reshape(1, feats),
            w_gate.T,
            w_up.T,
            w_down.T,
        )
        return result, new_state.reshape(rows, 1, head, head)

    return jax.shard_map(
        body,
        mesh=mesh,
        in_specs=(
            P("kv", "tp"),
            P(),
            P(None, "tp"),
            P(None, "tp"),
            P(None, "tp"),
            P(None, "tp"),
            P(None, None, "tp"),
            P("tp"),
            P("tp"),
            P("tp", None),
            P("kv", "tp", None, None),
            P(),
            P(None, ("kv", "tp")),
            P(None, ("kv", "tp")),
            P(None, ("kv", "tp")),
        ),
        out_specs=(P("kv", "tp"), P("kv", "tp", None, None)),
        check_vma=False,
    )
```

```python
import math

import jax
import jax.numpy as jnp
from jax import lax
from jax.experimental import pallas as pl
from jax.experimental.pallas import tpu as pltpu
from jax.sharding import PartitionSpec as P

EPS = 1e-06
MESH = pl.DeviceIdType.MESH
F32 = jnp.float32
BF16 = jnp.bfloat16


def layer_kernel(
    n_side,
    n_z,
    tok_hbm,
    again_hbm,
    wq_hbm,
    wk_hbm,
    wv_hbm,
    wo_hbm,
    wrates_hbm,
    hrate_ref,
    hgain_hbm,
    wout_hbm,
    state_hbm,
    mgain_hbm,
    wgate_hbm,
    wup_hbm,
    wdown_hbm,
    result_out,
    ns_out,
    tok_own,
    tok_all,
    wqkvg,
    wout,
    state,
    pred,
    again,
    mgain,
    hgain,
    wrates,
    own_w,
    far_w,
    gu,
    wd,
    part1,
    recv1,
    ag,
    ex_out,
    ex_in,
    exsq_out,
    exsq_in,
    pb,
    r1,
    mid,
    r2,
    zout,
    zin,
    local_sem,
    far_send_sem,
    far_recv_sem,
    tok_send_sem,
    tok_recv_sem,
    p1_send_sem,
    p1_recv_sem,
    agz_send_sem,
    agz_recv_sem,
    ag_send_sem,
    ag_recv_sem,
    ex_send_sem,
    ex_recv_sem,
    r_send_sem,
    r_recv_sem,
    rz_send_sem,
    rz_recv_sem,
):
    n_tp = 2 * n_z
    rows, fpd = tok_own.shape
    head = hgain.shape[1]
    units = own_w.shape[1]
    upad = gu.shape[1] // 4
    me_k = lax.axis_index("kv")
    me_t = lax.axis_index("tp")
    my_y, my_x = me_k // n_side, lax.rem(me_k, n_side)
    my_z, my_c = me_t // 2, lax.rem(me_t, 2)
    partner = me_t + 1 - 2 * my_c

    def z_at(d):
        return lax.rem(my_z + d, n_z)

    def y_at(d):
        return lax.rem(my_y + d, n_side)

    def x_at(d):
        return lax.rem(my_x + d, n_side)

    def tp_id(t):
        return {"tp": t}

    def kv_id(y, x):
        return {"kv": y * n_side + x}

    def local(src, dst, sem):
        cp = pltpu.make_async_copy(src, dst, sem)
        cp.start()
        return cp

    def send(src, dst, sent, received, device):
        pltpu.make_async_remote_copy(
            src_ref=src,
            dst_ref=dst,
            send_sem=sent,
            recv_sem=received,
            device_id=device,
            device_id_type=MESH,
        ).start()

    def await_bytes(like, sem):
        pltpu.make_async_copy(like, like, sem).wait()

    near = [0]
    for d in range(1, n_z // 2):
        near += [d, n_z - d]
    near += [n_z // 2]
    others = [(d, flip) for d in near for flip in (0, 1)][1:]
    side_far = [2, 1, 3] if n_side == 4 else list(range(1, n_side))
    side_near = side_far[1:] + side_far[:1]

    def tp_at(d, flip):
        c = (1 - my_c) if flip else my_c
        return z_at(d) * 2 + c

    def group_of(d):
        return 0 if min(d, n_z - d) <= 1 else (1 if min(d, n_z - d) == 2 else 2)

    tok_copy = local(tok_hbm, tok_own, local_sem.at[0])
    small = [
        local(again_hbm, again, local_sem.at[1]),
        local(mgain_hbm, mgain, local_sem.at[2]),
        local(hgain_hbm, hgain, local_sem.at[3]),
        local(wrates_hbm, wrates, local_sem.at[4]),
    ]
    mats = (wgate_hbm, wup_hbm, wdown_hbm)
    own_copies = [local(src, own_w.at[j], local_sem.at[5 + j]) for j, src in enumerate(mats)]
    w_copies = [
        local(src, wqkvg.at[:, pl.ds(j * head, head)], local_sem.at[8 + j])
        for j, src in enumerate((wq_hbm, wk_hbm, wv_hbm, wo_hbm))
    ]
    state_copy = local(state_hbm, state, local_sem.at[12])
    wout_copy = local(wout_hbm, wout, local_sem.at[13])

    barrier = pltpu.get_barrier_semaphore()
    for d, flip in reversed(others):
        pl.semaphore_signal(
            barrier, inc=1, device_id=tp_id(tp_at(d, flip)), device_id_type=MESH
        )
    for d in range(1, n_side):
        pl.semaphore_signal(
            barrier, inc=1, device_id=kv_id(y_at(d), my_x), device_id_type=MESH
        )
        pl.semaphore_signal(
            barrier, inc=1, device_id=kv_id(my_y, x_at(d)), device_id_type=MESH
        )
    tok_copy.wait()
    pl.semaphore_wait(barrier, len(others) + 2 * (n_side - 1))

    for d, flip in reversed(others):
        send(
            tok_own,
            tok_all.at[me_t],
            tok_send_sem,
            tok_recv_sem.at[group_of(d)],
            tp_id(tp_at(d, flip)),
        )

    for j, src in enumerate(mats):
        send(src, far_w.at[j], far_send_sem.at[j], far_recv_sem.at[j], tp_id(partner))

    for cp in small + w_copies:
        cp.wait()
    acc = jnp.zeros((rows, 4 * head), F32)
    square = jnp.zeros((rows, fpd), F32)
    write_sum = jnp.zeros((rows, fpd), F32)
    decay_sum = jnp.zeros((rows, fpd), F32)
    seen = set()
    for i, (d, flip) in enumerate([(0, 0)] + others):
        t = tp_at(d, flip)
        if i == 0:
            piece = tok_own[...].astype(F32)
        else:
            g = group_of(d)
            if g not in seen:
                seen.add(g)
                size = sum(group_of(e) == g for e, _ in others)
                await_bytes(tok_all.at[pl.ds(0, size)], tok_recv_sem.at[g])
            piece = tok_all[t].astype(F32)
        cols = pl.ds(pl.multiple_of(t * fpd, fpd), fpd)
        square += piece * piece
        lhs = (piece * again[:, cols]).astype(BF16)
        lhs32 = lhs.astype(F32)
        write_sum += lhs32 * wrates[0:1, cols].astype(F32)
        decay_sum += lhs32 * wrates[1:2, cols].astype(F32)
        acc += jnp.dot(lhs, wqkvg[cols, :], preferred_element_type=F32)
    count = fpd * n_tp
    scale = lax.rsqrt(jnp.sum(square, axis=1, keepdims=True) / count + EPS)
    acc = acc * scale
    query = acc[:, 0:head]
    key = acc[:, head : 2 * head]
    value = acc[:, 2 * head : 3 * head]
    gate_in = acc[:, 3 * head : 4 * head]
    write_raw = jnp.sum(write_sum, axis=1, keepdims=True) * scale
    decay_raw = jnp.sum(decay_sum, axis=1, keepdims=True) * scale
    unit_query = query * (
        lax.rsqrt(jnp.sum(query * query, axis=1, keepdims=True) + EPS) * head ** (-0.5)
    )
    unit_key = key * lax.rsqrt(jnp.sum(key * key, axis=1, keepdims=True) + EPS)
    strength = 1.0 / (1.0 + jnp.exp(-write_raw))
    softplus = jnp.maximum(decay_raw, 0.0) + jnp.log(1.0 + jnp.exp(-jnp.abs(decay_raw)))
    fade = jnp.exp(-hrate_ref[0] * softplus)

    state_copy.wait()
    stacked = jnp.concatenate(
        [unit_key, unit_query, jnp.zeros((head - 2 * rows, head), F32)], axis=0
    )
    turned = stacked.T
    for b in range(rows):
        block = state[b]
        pred[0, b : b + 1, :] = jnp.sum(turned[:, b : b + 1] * block, axis=0, keepdims=True)
        pred[1, b : b + 1, :] = jnp.sum(
            turned[:, rows + b : rows + b + 1] * block, axis=0, keepdims=True
        )
    fresh = strength * (value - fade * pred[0])
    overlap = jnp.sum(unit_query * unit_key, axis=1, keepdims=True)
    readout = fade * pred[1] + overlap * fresh
    normed_out = readout * lax.rsqrt(
        jnp.sum(readout * readout, axis=1, keepdims=True) / head + EPS
    )
    mixed = (normed_out * hgain[...] * (gate_in / (1.0 + jnp.exp(-gate_in)))).astype(BF16)

    wout_copy.wait()
    partial = jnp.dot(mixed, wout[...], preferred_element_type=F32).astype(BF16)
    for t in range(n_tp):
        part1[t] = partial[:, t * fpd : (t + 1) * fpd]
    for d, flip in reversed(others):
        to = tp_at(d, flip)
        send(part1.at[to], recv1.at[me_t], p1_send_sem, p1_recv_sem, tp_id(to))

    for b in range(rows):
        ns_out[b] = fade[b : b + 1, :] * state[b] + turned[:, b : b + 1] * fresh[b : b + 1, :]

    for cp in own_copies:
        cp.wait()
    for j in range(3):
        await_bytes(far_w.at[j], far_recv_sem.at[j])
    zero_rows = jnp.zeros((upad - units, fpd), BF16)
    for zz in range(n_z):
        cols = pl.ds(pl.multiple_of((2 * zz + my_c) * fpd, fpd), fpd)
        gain = mgain[:, cols]
        for s, src in enumerate((own_w, far_w)):
            for j in range(2):
                row = (2 * j + s) * upad
                scaled = (src[j, :, cols].astype(F32) * gain).astype(BF16)
                gu[zz, row : row + units, :] = scaled
                gu[zz, row + units : row + upad, :] = zero_rows
            wd[zz, s * upad : s * upad + units, :] = src[2, :, cols]
            wd[zz, s * upad + units : (s + 1) * upad, :] = zero_rows

    total = tok_own[...].astype(F32) + part1[me_t].astype(F32)
    await_bytes(recv1.at[pl.ds(0, n_tp - 1)], p1_recv_sem)
    for d, flip in others:
        total += recv1[tp_at(d, flip)].astype(F32)
    residual = total.astype(BF16)
    ag[my_z, my_y, my_x] = residual

    mine = ag.at[my_z, my_y, my_x]
    for d in reversed(near[1:]):
        back = (n_z - d) % n_z
        send(mine, mine, agz_send_sem, agz_recv_sem.at[back], tp_id(z_at(d) * 2 + my_c))

    def x_first(d):
        return near.index(d) % 2 == 0

    def first_to(d, e):
        return kv_id(my_y, x_at(e)) if x_first(d) else kv_id(y_at(e), my_x)

    def second_to(d, e):
        return kv_id(y_at(e), my_x) if x_first(d) else kv_id(my_y, x_at(e))

    def spread_own(d):
        block = ag.at[z_at(d), my_y, my_x]
        if d:
            await_bytes(block, agz_recv_sem.at[d])
        for e in side_far:
            send(block, block, ag_send_sem.at[0], ag_recv_sem.at[0, d], first_to(d, e))
        for e in side_far:
            send(block, block, ag_send_sem.at[1], ag_recv_sem.at[1, d], second_to(d, e))

    def spread_on(d):
        z = z_at(d)
        await_bytes(ag.at[z, 0, pl.ds(0, n_side - 1)], ag_recv_sem.at[0, d])
        for e in side_far:
            for f in side_near:
                block = ag.at[z, my_y, x_at(f)] if x_first(d) else ag.at[z, y_at(f), my_x]
                send(block, block, ag_send_sem.at[1], ag_recv_sem.at[1, d], second_to(d, e))

    batch = rows * n_side * n_side
    sums = [jnp.zeros((batch, 4 * upad), F32), jnp.zeros((batch, 128), F32)]

    def multiply(d):
        z = z_at(d)
        await_bytes(ag.at[z, pl.ds(0, n_side - 1)], ag_recv_sem.at[1, d])
        lhs = ag[z].reshape(batch, fpd)
        wide = lhs.astype(F32)
        wide = wide * wide
        for q in range(fpd // 128):
            sums[1] += wide[:, q * 128 : (q + 1) * 128]
        sums[0] += lax.dot_general(
            lhs, gu[z], (((1,), (1,)), ((), ())), preferred_element_type=F32
        )

    steps = (
        [(0, i) for i in range(3)]
        + [(1, 0)]
        + [(0, i) for i in range(3, n_z)]
        + [(1, i) for i in range(1, n_z)]
        + [(2, i) for i in range(n_z)]
    )
    for what, i in steps:
        (spread_own, spread_on, multiply)[what](near[i])

    ex_out[0] = sums[0][:, : 2 * upad].astype(BF16)
    ex_out[1] = sums[0][:, 2 * upad :].astype(BF16)
    exsq_out[...] = sums[1]
    send(ex_out, ex_in, ex_send_sem.at[0], ex_recv_sem.at[0], tp_id(partner))
    send(exsq_out, exsq_in, ex_send_sem.at[1], ex_recv_sem.at[1], tp_id(partner))
    await_bytes(ex_in, ex_recv_sem.at[0])
    await_bytes(exsq_in, ex_recv_sem.at[1])
    row_scale = lax.rsqrt(
        jnp.sum(sums[1] + exsq_in[...], axis=1, keepdims=True) / count + EPS
    )
    gate_far = pltpu.roll(ex_in[0].astype(F32), upad, 1)
    up_far = pltpu.roll(ex_in[1].astype(F32), upad, 1)
    gate_pre = (sums[0][:, : 2 * upad] + gate_far) * row_scale
    up_pre = (sums[0][:, 2 * upad :] + up_far) * row_scale
    hidden = (gate_pre / (1.0 + jnp.exp(-gate_pre)) * up_pre).astype(BF16)

    def send_first(d):
        z = z_at(d)
        for e in side_far:
            for f in side_near:
                if x_first(d):
                    block, slot, at = pb.at[z, y_at(e), x_at(f)], my_y, x_at(f)
                else:
                    block, slot, at = pb.at[z, y_at(f), x_at(e)], my_x, y_at(f)
                send(
                    block, r1.at[z, slot, at], r_send_sem.at[0], r_recv_sem.at[0, d],
                    second_to(d, e),
                )

    def sum_first(d):
        z = z_at(d)
        await_bytes(
            r1.at[z, pl.ds(0, n_side - 1), pl.ds(0, n_side - 1)], r_recv_sem.at[0, d]
        )
        for f in side_far:
            if x_first(d):
                block, place, at = pb[z, my_y, x_at(f)], y_at, x_at(f)
            else:
                block, place, at = pb[z, y_at(f), my_x], x_at, y_at(f)
            block = block.astype(F32)
            for e in side_near:
                block += r1[z, place(e), at].astype(F32)
            mid[z, at] = block.astype(BF16)

    def send_second(d):
        z = z_at(d)
        for e in side_far:
            at, slot = (x_at(e), my_x) if x_first(d) else (y_at(e), my_y)
            send(
                mid.at[z, at], r2.at[z, slot], r_send_sem.at[1], r_recv_sem.at[1, d],
                first_to(d, e),
            )
        for e in side_far:
            if x_first(d):
                block, slot = pb.at[z, y_at(e), my_x], r1.at[z, my_y, my_x]
            else:
                block, slot = pb.at[z, my_y, x_at(e)], r1.at[z, my_x, my_y]
            send(block, slot, r_send_sem.at[0], r_recv_sem.at[2, d], second_to(d, e))

    def sum_second(d):
        z = z_at(d)
        await_bytes(r2.at[z, pl.ds(0, n_side - 1)], r_recv_sem.at[1, d])
        await_bytes(r1.at[z, 0, pl.ds(0, n_side - 1)], r_recv_sem.at[2, d])
        first, me_first, second = (x_at, my_x, y_at) if x_first(d) else (y_at, my_y, x_at)
        block = pb[z, my_y, my_x].astype(F32)
        for e in side_near:
            block += r1[z, second(e), me_first].astype(F32)
        for e in side_near:
            block += r2[z, first(e)].astype(F32)
        zout[z] = block.astype(BF16)

    def send_third(d):
        if d:
            send(
                zout.at[z_at(d)], zin.at[my_z], rz_send_sem, rz_recv_sem,
                tp_id(z_at(d) * 2 + my_c),
            )

    far = list(reversed(near))
    for i, d in enumerate(far):
        z = z_at(d)
        down = jnp.dot(hidden, wd[z], preferred_element_type=F32)
        pb[z] = down.astype(BF16).reshape(n_side, n_side, rows, fpd)
        if i:
            send_first(far[i - 1])
    send_first(far[-1])
    lag = 4
    for i in range(n_z + lag + 1):
        if i < n_z:
            sum_first(far[i])
        if 0 <= i - 1 < n_z:
            send_second(far[i - 1])
        if 0 <= i - lag < n_z:
            sum_second(far[i - lag])
        if 0 <= i - lag - 1 < n_z:
            send_third(far[i - lag - 1])
    out = residual.astype(F32) + zout[my_z].astype(F32)
    await_bytes(zin.at[pl.ds(0, n_z - 1)], rz_recv_sem)
    for d in near[1:]:
        out += zin[z_at(d)].astype(F32)
    result_out[...] = out.astype(BF16)

    await_bytes(tok_all.at[pl.ds(0, n_tp - 1)], tok_send_sem)
    for j in range(3):
        await_bytes(far_w.at[j], far_send_sem.at[j])
    await_bytes(recv1.at[pl.ds(0, n_tp - 1)], p1_send_sem)
    await_bytes(zin.at[pl.ds(0, n_z - 1)], agz_send_sem)
    await_bytes(ag.at[:, 0, pl.ds(0, n_side - 1)], ag_send_sem.at[0])
    await_bytes(ag.at[:, pl.ds(0, n_side - 1)], ag_send_sem.at[1])
    await_bytes(ex_in, ex_send_sem.at[0])
    await_bytes(exsq_in, ex_send_sem.at[1])
    await_bytes(ag.at[:, pl.ds(0, n_side - 1)], r_send_sem.at[0])
    await_bytes(ag.at[:, 0, pl.ds(0, n_side - 1)], r_send_sem.at[1])
    await_bytes(zin.at[pl.ds(0, n_z - 1)], rz_send_sem)


def write_kernel(result_ref, ns_ref, result_out, ns_out, sem):
    copies = [
        pltpu.make_async_copy(ns_ref, ns_out, sem.at[0]),
        pltpu.make_async_copy(result_ref, result_out, sem.at[1]),
    ]
    for cp in copies:
        cp.start()
    for cp in copies:
        cp.wait()


def solution(mesh):
    n_kv, n_tp = mesh.shape["kv"], mesh.shape["tp"]
    n_side = math.isqrt(n_kv)
    n_z = n_tp // 2

    def body(
        tokens,
        attn_gain,
        w_query,
        w_key,
        w_value,
        w_outgate,
        w_rates,
        head_rate,
        head_gain,
        w_out,
        state,
        mlp_gain,
        w_gate,
        w_up,
        w_down,
    ):
        rows, fpd = tokens.shape
        feats = fpd * n_tp
        head = w_query.shape[1]
        units = w_gate.shape[1]
        upad = 64
        batch = rows * n_kv
        hbm = pl.BlockSpec(memory_space=pl.ANY)
        out_hbm = pl.BlockSpec(memory_space=pltpu.VMEM)
        smem = pl.BlockSpec(memory_space=pltpu.SMEM)
        dma = pltpu.SemaphoreType.DMA
        vmem = pltpu.VMEM

        def kernel(*refs):
            layer_kernel(n_side, n_z, *refs)

        operands = (
            tokens,
            attn_gain.reshape(1, feats),
            w_query,
            w_key,
            w_value,
            w_outgate,
            w_rates.reshape(2, feats),
            head_rate,
            head_gain.reshape(1, head),
            w_out,
            state.reshape(rows, head, head),
            mlp_gain.reshape(1, feats),
            w_gate.T,
            w_up.T,
            w_down.T,
        )
        operands = [
            a if a is head_rate else pltpu.with_memory_space_constraint(a, pltpu.HBM)
            for a in operands
        ]
        result, new_state = pl.pallas_call(
            kernel,
            name="layer",
            out_shape=(
                jax.ShapeDtypeStruct((rows, fpd), BF16),
                jax.ShapeDtypeStruct((rows, head, head), F32),
            ),
            in_specs=[hbm] * 7 + [smem] + [hbm] * 7,
            out_specs=(out_hbm, out_hbm),
            scratch_shapes=[
                vmem((rows, fpd), BF16),
                vmem((n_tp, rows, fpd), BF16),
                vmem((feats, 4 * head), BF16),
                vmem((head, feats), BF16),
                vmem((rows, head, head), F32),
                vmem((2, rows, head), F32),
                vmem((1, feats), F32),
                vmem((1, feats), F32),
                vmem((1, head), F32),
                vmem((2, feats), BF16),
                vmem((3, units, feats), BF16),
                vmem((3, units, feats), BF16),
                vmem((n_z, 4 * upad, fpd), BF16),
                vmem((n_z, 2 * upad, fpd), BF16),
                vmem((n_tp, rows, fpd), BF16),
                vmem((n_tp, rows, fpd), BF16),
                vmem((n_z, n_side, n_side, rows, fpd), BF16),
                vmem((2, batch, 2 * upad), BF16),
                vmem((2, batch, 2 * upad), BF16),
                vmem((batch, 128), F32),
                vmem((batch, 128), F32),
                vmem((n_z, n_side, n_side, rows, fpd), BF16),
                vmem((n_z, n_side, n_side, rows, fpd), BF16),
                vmem((n_z, n_side, rows, fpd), BF16),
                vmem((n_z, n_side, rows, fpd), BF16),
                vmem((n_z, rows, fpd), BF16),
                vmem((n_z, rows, fpd), BF16),
                dma((14,)),
                dma((3,)),
                dma((3,)),
                dma,
                dma((3,)),
                dma,
                dma,
                dma,
                dma((n_z,)),
                dma((2,)),
                dma((2, n_z)),
                dma((2,)),
                dma((2,)),
                dma((2,)),
                dma((3, n_z)),
                dma,
                dma,
            ],
            compiler_params=pltpu.CompilerParams(
                collective_id=0,
                has_side_effects=True,
                vmem_limit_bytes=50000 * 1024,
            ),
        )(*operands)
        result, new_state = pl.pallas_call(
            write_kernel,
            name="write",
            out_shape=(
                jax.ShapeDtypeStruct((rows, fpd), BF16),
                jax.ShapeDtypeStruct((rows, head, head), F32),
            ),
            in_specs=[pl.BlockSpec(memory_space=pltpu.VMEM)] * 2,
            out_specs=(pl.BlockSpec(memory_space=pl.ANY),) * 2,
            scratch_shapes=[dma((2,))],
            compiler_params=pltpu.CompilerParams(vmem_limit_bytes=4096 * 1024),
        )(result, new_state)
        return result, new_state.reshape(rows, 1, head, head)

    return jax.shard_map(
        body,
        mesh=mesh,
        in_specs=(
            P("kv", "tp"),
            P(),
            P(None, "tp"),
            P(None, "tp"),
            P(None, "tp"),
            P(None, "tp"),
            P(None, None, "tp"),
            P("tp"),
            P("tp"),
            P("tp", None),
            P("kv", "tp", None, None),
            P(),
            P(None, ("kv", "tp")),
            P(None, ("kv", "tp")),
            P(None, ("kv", "tp")),
        ),
        out_specs=(P("kv", "tp"), P("kv", "tp", None, None)),
        check_vma=False,
    )
```

```python
import math

import jax
import jax.numpy as jnp
from jax import lax
from jax.experimental import pallas as pl
from jax.experimental.pallas import tpu as pltpu
from jax.sharding import PartitionSpec as P

EPS = 1e-06
MESH = pl.DeviceIdType.MESH
F32 = jnp.float32
BF16 = jnp.bfloat16


def schedule(n_z, parts):
    every = range(n_z)
    steps = [("own", h, i) for i in range(3) for h in range(parts)]
    steps += [("on", h, 0) for h in range(parts)]
    steps += [("own", h, i) for i in range(3, n_z) for h in range(parts)]
    steps += [("on", h, i) for i in range(1, n_z) for h in range(parts)]
    for h in range(parts):
        steps += [("mm", h, i) for i in every] + [("swap", h), ("act", h)]
        for i in every:
            steps.append(("down", h, i))
            if i:
                steps.append(("s1", h, i - 1))
        steps.append(("s1", h, n_z - 1))
    lag = 8
    for h in range(parts):
        for i in range(n_z + lag + 1):
            if i < n_z:
                steps.append(("a1", h, i))
            if 0 <= i - 1 < n_z:
                steps.append(("s2", h, i - 1))
            if 0 <= i - lag < n_z:
                steps.append(("a2", h, i - lag))
            if 0 <= i - lag - 1 < n_z:
                steps.append(("s3", h, i - lag - 1))
    return steps


def layer_kernel(
    n_side,
    n_z,
    parts,
    tok_hbm,
    again_hbm,
    wq_hbm,
    wk_hbm,
    wv_hbm,
    wo_hbm,
    wrates_hbm,
    hrate_hbm,
    hgain_hbm,
    wout_hbm,
    state_hbm,
    mgain_hbm,
    wgate_hbm,
    wup_hbm,
    wdown_hbm,
    result_out,
    ns_out,
    tok_own,
    tok_all,
    wqkvg,
    wout,
    state,
    pred,
    again,
    mgain,
    hgain,
    hrate,
    wrates,
    own_w,
    far_w,
    gu,
    wd,
    part1,
    recv1,
    ag,
    ex_out,
    ex_in,
    exsq_out,
    exsq_in,
    pb,
    r1,
    mid,
    r2,
    zout,
    zin,
    local_sem,
    far_send_sem,
    far_recv_sem,
    tok_send_sem,
    tok_recv_sem,
    p1_send_sem,
    p1_recv_sem,
    agz_send_sem,
    agz_recv_sem,
    ag_send_sem,
    ag_recv_sem,
    ex_send_sem,
    ex_recv_sem,
    r_send_sem,
    r_recv_sem,
    rz_send_sem,
    rz_recv_sem,
):
    n_tp = 2 * n_z
    sub = ag.shape[4]
    rows, fpd = tok_own.shape
    head = hgain.shape[1]
    units = own_w.shape[1]
    upad = gu.shape[1] // 4
    me_k = lax.axis_index("kv")
    me_t = lax.axis_index("tp")
    my_y, my_x = me_k // n_side, lax.rem(me_k, n_side)
    my_z, my_c = me_t // 2, lax.rem(me_t, 2)
    partner = me_t + 1 - 2 * my_c

    def z_at(d):
        return lax.rem(my_z + d, n_z)

    def y_at(d):
        return lax.rem(my_y + d, n_side)

    def x_at(d):
        return lax.rem(my_x + d, n_side)

    def tp_id(t):
        return {"tp": t}

    def kv_id(y, x):
        return {"kv": y * n_side + x}

    def local(src, dst, sem):
        cp = pltpu.make_async_copy(src, dst, sem)
        cp.start()
        return cp

    def send(src, dst, sent, received, device):
        pltpu.make_async_remote_copy(
            src_ref=src,
            dst_ref=dst,
            send_sem=sent,
            recv_sem=received,
            device_id=device,
            device_id_type=MESH,
        ).start()

    def await_bytes(like, sem):
        pltpu.make_async_copy(like, like, sem).wait()

    near = [0]
    for d in range(1, n_z // 2):
        near += [d, n_z - d]
    near += [n_z // 2]
    others = [(d, flip) for d in near for flip in (0, 1)][1:]
    side_far = [2, 1, 3] if n_side == 4 else list(range(1, n_side))
    side_near = side_far[1:] + side_far[:1]

    def tp_at(d, flip):
        c = (1 - my_c) if flip else my_c
        return z_at(d) * 2 + c

    def group_of(d):
        return max(min(d, n_z - d) - 1, 0)

    tok_copy = local(tok_hbm, tok_own, local_sem.at[0])
    small = [
        local(again_hbm, again, local_sem.at[1]),
        local(mgain_hbm, mgain, local_sem.at[2]),
        local(hgain_hbm, hgain, local_sem.at[3]),
        local(wrates_hbm, wrates, local_sem.at[4]),
        local(hrate_hbm, hrate, local_sem.at[14]),
    ]
    mats = (wgate_hbm, wup_hbm, wdown_hbm)
    own_copies = [local(src, own_w.at[j], local_sem.at[5 + j]) for j, src in enumerate(mats)]
    w_copies = [
        local(src, wqkvg.at[:, pl.ds(j * head, head)], local_sem.at[8 + j])
        for j, src in enumerate((wq_hbm, wk_hbm, wv_hbm, wo_hbm))
    ]
    state_copy = local(state_hbm, state, local_sem.at[12])
    wout_copy = local(wout_hbm, wout, local_sem.at[13])

    barrier = pltpu.get_barrier_semaphore()
    for d, flip in reversed(others):
        pl.semaphore_signal(
            barrier, inc=1, device_id=tp_id(tp_at(d, flip)), device_id_type=MESH
        )
    for d in range(1, n_side):
        pl.semaphore_signal(
            barrier, inc=1, device_id=kv_id(y_at(d), my_x), device_id_type=MESH
        )
        pl.semaphore_signal(
            barrier, inc=1, device_id=kv_id(my_y, x_at(d)), device_id_type=MESH
        )
    tok_copy.wait()
    pl.semaphore_wait(barrier, len(others) + 2 * (n_side - 1))

    for d, flip in reversed(others):
        send(
            tok_own,
            tok_all.at[me_t],
            tok_send_sem,
            tok_recv_sem.at[group_of(d)],
            tp_id(tp_at(d, flip)),
        )

    for j, src in enumerate(mats):
        send(src, far_w.at[j], far_send_sem.at[j], far_recv_sem.at[j], tp_id(partner))

    for cp in small + w_copies:
        cp.wait()
    acc = jnp.zeros((rows, 4 * head), F32)
    square = jnp.zeros((rows, fpd), F32)
    write_sum = jnp.zeros((rows, fpd), F32)
    decay_sum = jnp.zeros((rows, fpd), F32)
    seen = set()
    for i, (d, flip) in enumerate([(0, 0)] + others):
        t = tp_at(d, flip)
        if i == 0:
            piece = tok_own[...].astype(F32)
        else:
            g = group_of(d)
            if g not in seen:
                seen.add(g)
                size = sum(group_of(e) == g for e, _ in others)
                await_bytes(tok_all.at[pl.ds(0, size)], tok_recv_sem.at[g])
            piece = tok_all[t].astype(F32)
        cols = pl.ds(pl.multiple_of(t * fpd, fpd), fpd)
        square += piece * piece
        lhs = (piece * again[:, cols]).astype(BF16)
        lhs32 = lhs.astype(F32)
        write_sum += lhs32 * wrates[0:1, cols].astype(F32)
        decay_sum += lhs32 * wrates[1:2, cols].astype(F32)
        acc += jnp.dot(lhs, wqkvg[cols, :], preferred_element_type=F32)
    count = fpd * n_tp
    scale = lax.rsqrt(jnp.sum(square, axis=1, keepdims=True) / count + EPS)
    acc = acc * scale
    query = acc[:, 0:head]
    key = acc[:, head : 2 * head]
    value = acc[:, 2 * head : 3 * head]
    gate_in = acc[:, 3 * head : 4 * head]
    write_raw = jnp.sum(write_sum, axis=1, keepdims=True) * scale
    decay_raw = jnp.sum(decay_sum, axis=1, keepdims=True) * scale
    unit_query = query * (
        lax.rsqrt(jnp.sum(query * query, axis=1, keepdims=True) + EPS) * head ** (-0.5)
    )
    unit_key = key * lax.rsqrt(jnp.sum(key * key, axis=1, keepdims=True) + EPS)
    strength = 1.0 / (1.0 + jnp.exp(-write_raw))
    softplus = jnp.maximum(decay_raw, 0.0) + jnp.log(1.0 + jnp.exp(-jnp.abs(decay_raw)))
    fade = jnp.exp(-hrate[:, 0:1] * softplus)

    state_copy.wait()
    stacked = jnp.concatenate(
        [unit_key, unit_query, jnp.zeros((head - 2 * rows, head), F32)], axis=0
    )
    turned = stacked.T
    for b in range(rows):
        block = state[b]
        pred[0, b : b + 1, :] = jnp.sum(turned[:, b : b + 1] * block, axis=0, keepdims=True)
        pred[1, b : b + 1, :] = jnp.sum(
            turned[:, rows + b : rows + b + 1] * block, axis=0, keepdims=True
        )
    fresh = strength * (value - fade * pred[0])
    overlap = jnp.sum(unit_query * unit_key, axis=1, keepdims=True)
    readout = fade * pred[1] + overlap * fresh
    normed_out = readout * lax.rsqrt(
        jnp.sum(readout * readout, axis=1, keepdims=True) / head + EPS
    )
    mixed = (normed_out * hgain[...] * (gate_in / (1.0 + jnp.exp(-gate_in)))).astype(BF16)

    wout_copy.wait()
    partial = jnp.dot(mixed, wout[...], preferred_element_type=F32).astype(BF16)
    for t in range(n_tp):
        part1[t] = partial[:, t * fpd : (t + 1) * fpd]
    for d, flip in reversed(others):
        to = tp_at(d, flip)
        send(part1.at[to], recv1.at[me_t], p1_send_sem, p1_recv_sem, tp_id(to))

    for b in range(rows):
        ns_out[b] = fade[b : b + 1, :] * state[b] + turned[:, b : b + 1] * fresh[b : b + 1, :]

    for cp in own_copies:
        cp.wait()
    for j in range(3):
        await_bytes(far_w.at[j], far_recv_sem.at[j])
    zero_rows = jnp.zeros((upad - units, fpd), BF16)
    for zz in range(n_z):
        cols = pl.ds(pl.multiple_of((2 * zz + my_c) * fpd, fpd), fpd)
        gain = mgain[:, cols]
        for s, src in enumerate((own_w, far_w)):
            for j in range(2):
                row = (2 * j + s) * upad
                scaled = (src[j, :, cols].astype(F32) * gain).astype(BF16)
                gu[zz, row : row + units, :] = scaled
                gu[zz, row + units : row + upad, :] = zero_rows
            wd[zz, s * upad : s * upad + units, :] = src[2, :, cols]
            wd[zz, s * upad + units : (s + 1) * upad, :] = zero_rows

    total = tok_own[...].astype(F32) + part1[me_t].astype(F32)
    await_bytes(recv1.at[pl.ds(0, n_tp - 1)], p1_recv_sem)
    for d, flip in others:
        total += recv1[tp_at(d, flip)].astype(F32)
    residual = total.astype(BF16)
    for h in range(parts):
        ag[h, my_z, my_y, my_x] = residual[h * sub : (h + 1) * sub, :]

    mine = ag.at[:, my_z, my_y, my_x]
    for d in reversed(near[1:]):
        back = (n_z - d) % n_z
        send(mine, mine, agz_send_sem, agz_recv_sem.at[back], tp_id(z_at(d) * 2 + my_c))

    def x_first(d):
        return near.index(d) % 2 == 0

    def first_to(d, e):
        return kv_id(my_y, x_at(e)) if x_first(d) else kv_id(y_at(e), my_x)

    def second_to(d, e):
        return kv_id(y_at(e), my_x) if x_first(d) else kv_id(my_y, x_at(e))

    def spread_own(h, d):
        z = z_at(d)
        block = ag.at[h, z, my_y, my_x]
        if d and h == 0:
            await_bytes(ag.at[:, z, my_y, my_x], agz_recv_sem.at[d])
        for e in side_far:
            send(block, block, ag_send_sem.at[0], ag_recv_sem.at[0, h, d], first_to(d, e))
        for e in side_far:
            send(block, block, ag_send_sem.at[1], ag_recv_sem.at[1, h, d], second_to(d, e))

    def spread_on(h, d):
        z = z_at(d)
        await_bytes(ag.at[h, z, 0, pl.ds(0, n_side - 1)], ag_recv_sem.at[0, h, d])
        for e in side_far:
            for f in side_near:
                if x_first(d):
                    block = ag.at[h, z, my_y, x_at(f)]
                else:
                    block = ag.at[h, z, y_at(f), my_x]
                send(
                    block, block, ag_send_sem.at[1], ag_recv_sem.at[1, h, d], second_to(d, e)
                )

    batch = sub * n_side * n_side
    gate_up = [jnp.zeros((batch, 4 * upad), F32) for _ in range(parts)]
    squares = [jnp.zeros((batch, 128), F32) for _ in range(parts)]
    hidden = [None] * parts

    def multiply(h, d):
        z = z_at(d)
        await_bytes(ag.at[h, z, pl.ds(0, n_side - 1)], ag_recv_sem.at[1, h, d])
        lhs = ag[h, z].reshape(batch, fpd)
        wide = lhs.astype(F32)
        wide = wide * wide
        for q in range(fpd // 128):
            squares[h] += wide[:, q * 128 : (q + 1) * 128]
        gate_up[h] += lax.dot_general(
            lhs, gu[z], (((1,), (1,)), ((), ())), preferred_element_type=F32
        )

    def swap(h):
        ex_out[h, 0] = gate_up[h][:, : 2 * upad].astype(BF16)
        ex_out[h, 1] = gate_up[h][:, 2 * upad :].astype(BF16)
        exsq_out[h] = squares[h]
        send(ex_out.at[h], ex_in.at[h], ex_send_sem.at[0, h], ex_recv_sem.at[0, h], tp_id(partner))
        send(
            exsq_out.at[h], exsq_in.at[h], ex_send_sem.at[1, h], ex_recv_sem.at[1, h],
            tp_id(partner),
        )

    def activate(h):
        await_bytes(ex_in.at[h], ex_recv_sem.at[0, h])
        await_bytes(exsq_in.at[h], ex_recv_sem.at[1, h])
        row_scale = lax.rsqrt(
            jnp.sum(squares[h] + exsq_in[h], axis=1, keepdims=True) / count + EPS
        )
        gate_far = pltpu.roll(ex_in[h, 0].astype(F32), upad, 1)
        up_far = pltpu.roll(ex_in[h, 1].astype(F32), upad, 1)
        gate_pre = (gate_up[h][:, : 2 * upad] + gate_far) * row_scale
        up_pre = (gate_up[h][:, 2 * upad :] + up_far) * row_scale
        hidden[h] = (gate_pre / (1.0 + jnp.exp(-gate_pre)) * up_pre).astype(BF16)

    def project(h, d):
        z = z_at(d)
        down = jnp.dot(hidden[h], wd[z], preferred_element_type=F32)
        pb[h, z] = down.astype(BF16).reshape(n_side, n_side, sub, fpd)

    def send_first(h, d):
        z = z_at(d)
        for e in side_far:
            for f in side_near:
                if x_first(d):
                    block, slot, at = pb.at[h, z, y_at(e), x_at(f)], my_y, x_at(f)
                else:
                    block, slot, at = pb.at[h, z, y_at(f), x_at(e)], my_x, y_at(f)
                send(
                    block, r1.at[h, z, slot, at], r_send_sem.at[0], r_recv_sem.at[0, h, d],
                    second_to(d, e),
                )

    def sum_first(h, d):
        z = z_at(d)
        await_bytes(
            r1.at[h, z, pl.ds(0, n_side - 1), pl.ds(0, n_side - 1)], r_recv_sem.at[0, h, d]
        )
        for f in side_far:
            if x_first(d):
                block, place, at = pb[h, z, my_y, x_at(f)], y_at, x_at(f)
            else:
                block, place, at = pb[h, z, y_at(f), my_x], x_at, y_at(f)
            block = block.astype(F32)
            for e in side_near:
                block += r1[h, z, place(e), at].astype(F32)
            mid[h, z, at] = block.astype(BF16)

    def send_second(h, d):
        z = z_at(d)
        for e in side_far:
            at, slot = (x_at(e), my_x) if x_first(d) else (y_at(e), my_y)
            send(
                mid.at[h, z, at], r2.at[h, z, slot], r_send_sem.at[1], r_recv_sem.at[1, h, d],
                first_to(d, e),
            )
        for e in side_far:
            if x_first(d):
                block, slot = pb.at[h, z, y_at(e), my_x], r1.at[h, z, my_y, my_x]
            else:
                block, slot = pb.at[h, z, my_y, x_at(e)], r1.at[h, z, my_x, my_y]
            send(block, slot, r_send_sem.at[0], r_recv_sem.at[2, h, d], second_to(d, e))

    def sum_second(h, d):
        z = z_at(d)
        await_bytes(r2.at[h, z, pl.ds(0, n_side - 1)], r_recv_sem.at[1, h, d])
        await_bytes(r1.at[h, z, 0, pl.ds(0, n_side - 1)], r_recv_sem.at[2, h, d])
        first, me_first, second = (x_at, my_x, y_at) if x_first(d) else (y_at, my_y, x_at)
        block = pb[h, z, my_y, my_x].astype(F32)
        for e in side_near:
            block += r1[h, z, second(e), me_first].astype(F32)
        for e in side_near:
            block += r2[h, z, first(e)].astype(F32)
        zout[h, z] = block.astype(BF16)

    def send_third(h, d):
        if d:
            send(
                zout.at[h, z_at(d)], zin.at[h, my_z], rz_send_sem, rz_recv_sem.at[h],
                tp_id(z_at(d) * 2 + my_c),
            )

    actions = {
        "own": spread_own,
        "on": spread_on,
        "mm": multiply,
        "swap": swap,
        "act": activate,
        "down": project,
        "s1": send_first,
        "a1": sum_first,
        "s2": send_second,
        "a2": sum_second,
        "s3": send_third,
    }
    far = list(reversed(near))
    for what, h, *which in schedule(n_z, parts):
        if which:
            order = far if what in ("down", "s1", "a1", "s2", "a2", "s3") else near
            actions[what](h, order[which[0]])
        else:
            actions[what](h)

    for h in range(parts):
        out = residual[h * sub : (h + 1) * sub, :].astype(F32) + zout[h, my_z].astype(F32)
        await_bytes(zin.at[h, pl.ds(0, n_z - 1)], rz_recv_sem.at[h])
        for d in near[1:]:
            out += zin[h, z_at(d)].astype(F32)
        result_out[h * sub : (h + 1) * sub, :] = out.astype(BF16)

    await_bytes(tok_all.at[pl.ds(0, n_tp - 1)], tok_send_sem)
    for j in range(3):
        await_bytes(far_w.at[j], far_send_sem.at[j])
    await_bytes(recv1.at[pl.ds(0, n_tp - 1)], p1_send_sem)
    await_bytes(zin.at[:, pl.ds(0, n_z - 1)], agz_send_sem)
    await_bytes(ag.at[:, :, 0, pl.ds(0, n_side - 1)], ag_send_sem.at[0])
    await_bytes(ag.at[:, :, pl.ds(0, n_side - 1)], ag_send_sem.at[1])
    for h in range(parts):
        await_bytes(ex_in.at[h], ex_send_sem.at[0, h])
        await_bytes(exsq_in.at[h], ex_send_sem.at[1, h])
    await_bytes(ag.at[:, :, pl.ds(0, n_side - 1)], r_send_sem.at[0])
    await_bytes(ag.at[:, :, 0, pl.ds(0, n_side - 1)], r_send_sem.at[1])
    await_bytes(zin.at[:, pl.ds(0, n_z - 1)], rz_send_sem)


def write_kernel(result_ref, ns_ref, result_out, ns_out, sem):
    copies = [
        pltpu.make_async_copy(ns_ref, ns_out, sem.at[0]),
        pltpu.make_async_copy(result_ref, result_out, sem.at[1]),
    ]
    for cp in copies:
        cp.start()
    for cp in copies:
        cp.wait()


def solution(mesh):
    n_kv, n_tp = mesh.shape["kv"], mesh.shape["tp"]
    n_side = math.isqrt(n_kv)
    n_z = n_tp // 2

    def body(
        tokens,
        attn_gain,
        w_query,
        w_key,
        w_value,
        w_outgate,
        w_rates,
        head_rate,
        head_gain,
        w_out,
        state,
        mlp_gain,
        w_gate,
        w_up,
        w_down,
    ):
        rows, fpd = tokens.shape
        feats = fpd * n_tp
        head = w_query.shape[1]
        units = w_gate.shape[1]
        upad = 64
        parts = 1
        sub = rows // parts
        batch = sub * n_kv
        hbm = pl.BlockSpec(memory_space=pl.ANY)
        out_hbm = pl.BlockSpec(memory_space=pltpu.VMEM)
        dma = pltpu.SemaphoreType.DMA
        vmem = pltpu.VMEM

        def kernel(*refs):
            layer_kernel(n_side, n_z, parts, *refs)

        operands = (
            tokens,
            attn_gain.reshape(1, feats),
            w_query,
            w_key,
            w_value,
            w_outgate,
            w_rates.reshape(2, feats),
            head_rate.reshape(1, 1),
            head_gain.reshape(1, head),
            w_out,
            state.reshape(rows, head, head),
            mlp_gain.reshape(1, feats),
            w_gate.T,
            w_up.T,
            w_down.T,
        )
        operands = [
            pltpu.with_memory_space_constraint(a, pltpu.HBM) if a.size > 1 else a
            for a in operands
        ]
        result, new_state = pl.pallas_call(
            kernel,
            name="layer",
            out_shape=(
                jax.ShapeDtypeStruct((rows, fpd), BF16),
                jax.ShapeDtypeStruct((rows, head, head), F32),
            ),
            in_specs=[hbm] * 15,
            out_specs=(out_hbm, out_hbm),
            scratch_shapes=[
                vmem((rows, fpd), BF16),
                vmem((n_tp, rows, fpd), BF16),
                vmem((feats, 4 * head), BF16),
                vmem((head, feats), BF16),
                vmem((rows, head, head), F32),
                vmem((2, rows, head), F32),
                vmem((1, feats), F32),
                vmem((1, feats), F32),
                vmem((1, head), F32),
                vmem((1, 1), F32),
                vmem((2, feats), BF16),
                vmem((3, units, feats), BF16),
                vmem((3, units, feats), BF16),
                vmem((n_z, 4 * upad, fpd), BF16),
                vmem((n_z, 2 * upad, fpd), BF16),
                vmem((n_tp, rows, fpd), BF16),
                vmem((n_tp, rows, fpd), BF16),
                vmem((parts, n_z, n_side, n_side, sub, fpd), BF16),
                vmem((parts, 2, batch, 2 * upad), BF16),
                vmem((parts, 2, batch, 2 * upad), BF16),
                vmem((parts, batch, 128), F32),
                vmem((parts, batch, 128), F32),
                vmem((parts, n_z, n_side, n_side, sub, fpd), BF16),
                vmem((parts, n_z, n_side, n_side, sub, fpd), BF16),
                vmem((parts, n_z, n_side, sub, fpd), BF16),
                vmem((parts, n_z, n_side, sub, fpd), BF16),
                vmem((parts, n_z, sub, fpd), BF16),
                vmem((parts, n_z, sub, fpd), BF16),
                dma((15,)),
                dma((3,)),
                dma((3,)),
                dma,
                dma((n_z // 2,)),
                dma,
                dma,
                dma,
                dma((n_z,)),
                dma((2,)),
                dma((2, parts, n_z)),
                dma((2, parts)),
                dma((2, parts)),
                dma((2,)),
                dma((3, parts, n_z)),
                dma,
                dma((parts,)),
            ],
            compiler_params=pltpu.CompilerParams(
                collective_id=0,
                has_side_effects=True,
                vmem_limit_bytes=50000 * 1024,
            ),
        )(*operands)
        result, new_state = pl.pallas_call(
            write_kernel,
            name="write",
            out_shape=(
                jax.ShapeDtypeStruct((rows, fpd), BF16),
                jax.ShapeDtypeStruct((rows, head, head), F32),
            ),
            in_specs=[pl.BlockSpec(memory_space=pltpu.VMEM)] * 2,
            out_specs=(pl.BlockSpec(memory_space=pl.ANY),) * 2,
            scratch_shapes=[dma((2,))],
            compiler_params=pltpu.CompilerParams(vmem_limit_bytes=4096 * 1024),
        )(result, new_state)
        return result, new_state.reshape(rows, 1, head, head)

    return jax.shard_map(
        body,
        mesh=mesh,
        in_specs=(
            P("kv", "tp"),
            P(),
            P(None, "tp"),
            P(None, "tp"),
            P(None, "tp"),
            P(None, "tp"),
            P(None, None, "tp"),
            P("tp"),
            P("tp"),
            P("tp", None),
            P("kv", "tp", None, None),
            P(),
            P(None, ("kv", "tp")),
            P(None, ("kv", "tp")),
            P(None, ("kv", "tp")),
        ),
        out_specs=(P("kv", "tp"), P("kv", "tp", None, None)),
        check_vma=False,
    )
```
